512 devices in a mesh: kv: 64 (over z, y), tp: 8 (over x, core).
Axes of the slice: x: 4, y: 8, z: 8, core: 2. Of those that a mesh axis runs over, the one named last changes fastest.
Arguments:
- tokens: bfloat16 [1024, 2048], P('kv', 'tp'), may hold values from -20 to 20
- norm_gain: float32 [2048], replicated, may hold values from 0.1 to 1.9
- w_query: bfloat16 [2048, 1024], P(None, 'tp'), may hold values from -0.125 to 0.125
- w_key: bfloat16 [2048, 1024], P(None, 'tp'), may hold values from -0.125 to 0.125
- w_value: bfloat16 [2048, 1024], P(None, 'tp'), may hold values from -0.125 to 0.125
- w_outgate: bfloat16 [2048, 1024], P(None, 'tp'), may hold values from -0.125 to 0.125
- w_input_gate: bfloat16 [2048, 8], replicated, may hold values from -0.125 to 0.125
- w_forget_gate: bfloat16 [2048, 8], replicated, may hold values from -0.125 to 0.125
- memory: float32 [1024, 8, 128, 128], P('kv', 'tp'), may hold values from -6 to 6
- normalizer: float32 [1024, 8, 128], P('kv', 'tp'), may hold values from -6 to 6
- memory_max: float32 [1024, 8], P('kv', 'tp'), may hold values from -2 to 300
- w_output: bfloat16 [1024, 2048], P(None, 'tp'), may hold values from -0.1875 to 0.1875
- ffn_gain: float32 [2048], P('tp'), may hold values from 0.1 to 1.9
- w_gate: bfloat16 [2048, 5632], P('tp', 'kv'), may hold values from -0.125 to 0.125
- w_up: bfloat16 [2048, 5632], P('tp', 'kv'), may hold values from -0.125 to 0.125
- w_down: bfloat16 [5632, 2048], P('kv', 'tp'), may hold values from -0.078125 to 0.078125
Outputs:
- result: bfloat16 [1024, 2048], P('kv', 'tp')
- new_memory: float32 [1024, 8, 128, 128], P('kv', 'tp')
- new_normalizer: float32 [1024, 8, 128], P('kv', 'tp')
- new_max: float32 [1024, 8], P('kv', 'tp')
The draws below stay inside these ranges and needn't reach their ends.
All inputs are finite; a program needn't handle non-finite values.
Results may differ from the reference program's by a relative error of at most 0.013.
Values may be sent and summed in bfloat16 or wider, within the bound.
A program may use at most 64 MiB of HBM per device.

```python
import jax
import jax.numpy as jnp
from jax import lax

D = 2048
HEADS = 8
HEAD_DIM = 128
INNER = 1024
FF = 5632
BATCH = 1024


def draw_tokens(key, part):
    key_list = jax.random.split(jax.random.fold_in(key, 11), 3)
    col_pos = jnp.arange(D, dtype=jnp.float32) / (D - 1)
    col_jitter = jnp.exp(jax.random.uniform(key_list[2], (D,), jnp.float32, jnp.log(0.7), jnp.log(1.4)))
    base_draw = jnp.clip(jax.random.normal(key_list[0], (BATCH, D), jnp.float32), -4.0, 4.0)
    rise_curve = 0.6 * jnp.exp(col_pos * jnp.log(3.0))
    row_factor = jnp.exp(jax.random.uniform(key_list[1], (BATCH,), jnp.float32, jnp.log(0.5), jnp.log(2.0)))
    full_draw = base_draw * row_factor[:, None] * (rise_curve * col_jitter)[None, :]
    return jnp.clip(full_draw, -20.0, 20.0).astype(jnp.bfloat16)


def draw_memory_max(key, part):
    key_list = jax.random.split(jax.random.fold_in(key, 23), 1)
    base_draw = jax.random.uniform(key_list[0], (BATCH, HEADS), jnp.float32, -2.0, 2.0)
    return base_draw.astype(jnp.float32)


def shard_levels(own_key, extent, cuts, low, largest):
    loudness, own = 1.0, jax.random.fold_in(own_key, 6)
    for position, blocks in cuts:
        draws = jnp.exp(jax.random.uniform(jax.random.fold_in(own, position), (blocks,), jnp.float32, low / len(cuts), largest / len(cuts)))
        loudness = loudness * jnp.repeat(draws, extent[position] // blocks).reshape([-1 if axis == position else 1 for axis in range(len(extent))])
    return loudness


def scatter_about(rng, dims, scale, reach, pieces=(), held_as=jnp.bfloat16):
    drawn = scale * jax.random.normal(rng, dims, jnp.float32)
    if pieces:
        drawn = drawn * shard_levels(rng, dims, pieces, -0.22, 0.18)
    return jnp.clip(drawn, -reach, reach).astype(held_as)


def setup_inputs(seed: int = 0) -> dict:
    seeds = jax.random.split(jax.random.key(seed), 17)
    tokens = draw_tokens(jax.random.fold_in(seeds[16], 71), 0)
    norm_gain = jnp.clip(1.0 + 0.18 * jax.random.normal(seeds[1], (D,), jnp.float32), 0.1, 1.9)
    w_query = scatter_about(seeds[2], (D, INNER), D ** -0.5, 0.125, ((1, 8),))
    w_key = scatter_about(seeds[3], (D, INNER), D ** -0.5, 0.125, ((1, 8),))
    w_value = scatter_about(seeds[4], (D, INNER), D ** -0.5, 0.125, ((1, 8),))
    w_outgate = scatter_about(seeds[5], (D, INNER), D ** -0.5, 0.125, ((1, 8),))
    w_input_gate = scatter_about(seeds[6], (D, HEADS), D ** -0.5, 0.125)
    w_forget_gate = scatter_about(seeds[7], (D, HEADS), D ** -0.5, 0.125)
    memory = scatter_about(seeds[8], (BATCH, HEADS, HEAD_DIM, HEAD_DIM), 1.0, 6.0, ((0, 64), (1, 8)), jnp.float32)
    normalizer = scatter_about(seeds[9], (BATCH, HEADS, HEAD_DIM), 1.0, 6.0, ((0, 64), (1, 8)), jnp.float32)
    memory_max = draw_memory_max(jax.random.fold_in(seeds[16], 71), 0)
    w_output = scatter_about(seeds[11], (INNER, D), INNER ** -0.5, 0.1875, ((1, 8),))
    ffn_gain = jnp.clip(1.0 + 0.18 * jax.random.normal(seeds[12], (D,), jnp.float32), 0.1, 1.9)
    w_gate = scatter_about(seeds[13], (D, FF), D ** -0.5, 0.125, ((0, 8), (1, 64)))
    w_up = scatter_about(seeds[14], (D, FF), D ** -0.5, 0.125, ((0, 8), (1, 64)))
    w_down = scatter_about(seeds[15], (FF, D), FF ** -0.5, 0.078125, ((0, 64), (1, 8)))
    return dict(tokens=tokens, norm_gain=norm_gain, w_query=w_query, w_key=w_key, w_value=w_value, w_outgate=w_outgate, w_input_gate=w_input_gate, w_forget_gate=w_forget_gate, memory=memory, normalizer=normalizer, memory_max=memory_max, w_output=w_output, ffn_gain=ffn_gain, w_gate=w_gate, w_up=w_up, w_down=w_down)


def reference(tokens, norm_gain, w_query, w_key, w_value, w_outgate, w_input_gate, w_forget_gate, memory, normalizer, memory_max, w_output, ffn_gain, w_gate, w_up, w_down):
    tokens_f = tokens.astype(jnp.float32)
    row_scale = lax.rsqrt(lax.optimization_barrier(jnp.mean(tokens_f * tokens_f, axis=-1, keepdims=True)) + 1e-06)
    normed = (tokens_f * row_scale * norm_gain).astype(jnp.bfloat16)

    def project(weight):
        return jnp.dot(normed, weight, preferred_element_type=jnp.float32).reshape(BATCH, HEADS, HEAD_DIM)
    queries = project(w_query) * HEAD_DIM ** (-0.5)
    key_vec = project(w_key)
    values = project(w_value)
    outgate = project(w_outgate)
    igate = jnp.dot(normed, w_input_gate, preferred_element_type=jnp.float32)
    lforget = jax.nn.log_sigmoid(jnp.dot(normed, w_forget_gate, preferred_element_type=jnp.float32))
    new_max = jnp.maximum(lforget + memory_max, igate)
    keep_weight = jnp.exp(lforget + memory_max - new_max)
    admit_weight = jnp.exp(igate - new_max)
    new_memory = keep_weight[..., None, None] * memory + admit_weight[..., None, None] * (key_vec[..., :, None] * values[..., None, :])
    new_normalizer = keep_weight[..., None] * normalizer + admit_weight[..., None] * key_vec
    numerator = jnp.einsum('bhd,bhdv->bhv', queries, new_memory, precision=lax.Precision.HIGHEST)
    denominator = lax.optimization_barrier(jnp.sum(queries * new_normalizer, axis=-1))
    cell_out = numerator / jnp.maximum(jnp.abs(denominator), jnp.exp(-new_max))[..., None]
    head_mean = lax.optimization_barrier(jnp.mean(cell_out, axis=-1, keepdims=True))
    centered = cell_out - head_mean
    head_var = lax.optimization_barrier(jnp.mean(centered * centered, axis=-1, keepdims=True))
    mixed = (jax.nn.sigmoid(outgate) * centered * lax.rsqrt(head_var + 1e-05)).reshape(BATCH, INNER).astype(jnp.bfloat16)
    resid = (tokens_f + jnp.dot(mixed, w_output, preferred_element_type=jnp.float32)).astype(jnp.bfloat16)
    resid_f = resid.astype(jnp.float32)
    ffn_scale = lax.rsqrt(lax.optimization_barrier(jnp.mean(resid_f * resid_f, axis=-1, keepdims=True)) + 1e-06)
    ffn_in = (resid_f * ffn_gain).astype(jnp.bfloat16)
    gate_act = ffn_scale * jnp.dot(ffn_in, w_gate, preferred_element_type=jnp.float32)
    up_act = ffn_scale * jnp.dot(ffn_in, w_up, preferred_element_type=jnp.float32)
    hidden = (jax.nn.silu(gate_act) * up_act).astype(jnp.bfloat16)
    result = (resid_f + jnp.dot(hidden, w_down, preferred_element_type=jnp.float32)).astype(jnp.bfloat16)
    return (result, new_memory, new_normalizer, new_max)
```

```python
import functools

import jax
import jax.numpy as jnp
from jax import lax
from jax.experimental import pallas as pl
from jax.experimental.pallas import tpu as pltpu
from jax.sharding import PartitionSpec as P

EPS = 1e-06
HEAD_EPS = 1e-05
F32 = jnp.float32
BF16 = jnp.bfloat16
MESH = pl.DeviceIdType.MESH


def transposed_rhs(a, b):
    return lax.dot_general(a, b, (((1,), (1,)), ((), ())), preferred_element_type=F32)


def near_first(n):
    order = [0]
    for step in range(1, n // 2 + 1):
        order += [step] if step == n - step else [step, n - step]
    return order


def kernel(
    Z, Y, T, S, SHARD, PAD,
    tok_hbm, ngain_hbm, wq_hbm, wk_hbm, wv_hbm, wo_hbm, wig_hbm, wfg_hbm,
    mem_hbm, nrm_hbm, mmax_hbm, wout_hbm, fgain_hbm, wg_hbm, wu_hbm, wd_hbm,
    res_hbm, newmem_hbm, newnrm_hbm, newmax_hbm,
    tok, ngain, wproj, wgates, mem, nrm, mmax, wout, fgain, wgu, wd,
    newmem, newnrm, newmax, num, mixed, rows, csend, cbuf, hid, esend, ebuf, outv,
    load_sem, out_sem, a_send, a_recv, w_send, w_recv, m_send, m_recv, b_send, b_recv,
    c_send, c_recv, d_send, d_recv, e_send, e_recv,
):
    kv = lax.axis_index("kv")
    t = lax.axis_index("tp")
    z, y = kv // Y, kv % Y
    par = z % 2
    base = z - par
    R, CH = tok.shape[1], tok.shape[2]
    HD = mem.shape[1]
    width = T * CH
    GH = S * PAD

    def tp_peer(step):
        return (kv, (t + step) % T)

    def row_peer(dz, dy):
        return ((base + (par + dz) % 2) * Y + (y + dy) % Y, t)

    def weight_peer(step):
        return (((z + 2 * step) % Z) * Y + y, t)

    for s in range(S):
        for i in range(2):
            wgu[i, s, SHARD:PAD, :] = jnp.zeros((PAD - SHARD, CH), BF16)
        wd[s, SHARD:PAD, :] = jnp.zeros((PAD - SHARD, CH), BF16)
    loads = {}

    def load(name, src, dst):
        copy = pltpu.make_async_copy(src, dst, load_sem.at[len(loads)])
        copy.start()
        loads[name] = copy

    load("tok", tok_hbm, tok.at[t])
    load("wg", wg_hbm, wgu.at[0, 0, pl.ds(0, SHARD)])
    load("wu", wu_hbm, wgu.at[1, 0, pl.ds(0, SHARD)])
    load("wd", wd_hbm, wd.at[0, pl.ds(0, SHARD)])
    load("ngain", ngain_hbm, ngain)
    for i, w in enumerate((wq_hbm, wk_hbm, wv_hbm, wo_hbm)):
        load(f"w{i}", w, wproj.at[:, pl.ds(i * HD, HD)])
    load("wig", wig_hbm, wgates.at[0])
    load("wfg", wfg_hbm, wgates.at[1])
    load("mmax", mmax_hbm, mmax)
    load("nrm", nrm_hbm, nrm)
    load("mem", mem_hbm, mem)
    load("wout", wout_hbm, wout)
    load("fgain", fgain_hbm, fgain)

    barrier = pltpu.get_barrier_semaphore()
    peers = [tp_peer(step) for step in range(1, T)]
    peers += [row_peer(dz, dy) for dy in range(Y) for dz in range(2) if dz or dy]
    peers += [weight_peer(step) for step in range(1, S)]
    for peer in peers:
        pl.semaphore_signal(barrier, inc=1, device_id=peer, device_id_type=MESH)
    loads["tok"].wait()
    loads["wg"].wait()
    loads["wu"].wait()
    loads["wd"].wait()
    pl.semaphore_wait(barrier, len(peers))

    def send(src, dst, ssem, rsem, peer):
        copy = pltpu.make_async_remote_copy(
            src_ref=src, dst_ref=dst, send_sem=ssem, recv_sem=rsem,
            device_id=peer, device_id_type=MESH,
        )
        return copy

    a_copies = []
    for step in range(1, T):
        copy = send(tok.at[t], tok.at[t], a_send.at[step], a_recv.at[step], tp_peer(step))
        copy.start()
        a_copies.append(copy)
    w_copies = {}
    for i in range(3):
        for step in range(1, S):
            if i < 2:
                src, dst = wgu.at[i, 0, pl.ds(0, SHARD)], wgu.at[i, step, pl.ds(0, SHARD)]
            else:
                src, dst = wd.at[0, pl.ds(0, SHARD)], wd.at[step, pl.ds(0, SHARD)]
            copy = send(src, dst, w_send.at[i, step], w_recv.at[i, step], weight_peer(step))
            copy.start()
            w_copies[i, step] = copy

    for name in ("ngain", "w0", "w1", "w2", "w3", "wig", "wfg", "mmax", "nrm", "mem"):
        loads[name].wait()
    for copy in a_copies:
        copy.wait_recv()

    blocks = [tok[i].astype(F32) for i in range(T)]
    square = sum(jnp.sum(b * b, axis=-1, keepdims=True) for b in blocks)
    row_scale = lax.rsqrt(square / width + EPS)
    proj = jnp.zeros((R, 4 * HD), F32)
    ipre = jnp.zeros((R, wgates.shape[1]), F32)
    fpre = jnp.zeros((R, wgates.shape[1]), F32)
    for i in range(T):
        cols = slice(i * CH, (i + 1) * CH)
        normed = (blocks[i] * row_scale * ngain[:, cols]).astype(BF16)
        proj += jnp.dot(normed, wproj[cols, :], preferred_element_type=F32)
        ipre += transposed_rhs(normed, wgates[0, :, cols])
        fpre += transposed_rhs(normed, wgates[1, :, cols])
    queries = proj[:, :HD] * HD ** (-0.5)
    key_vec = proj[:, HD : 2 * HD]
    values = proj[:, 2 * HD : 3 * HD]
    outgate = proj[:, 3 * HD :]
    mine = lax.broadcasted_iota(jnp.int32, ipre.shape, 1) == t
    igate = jnp.sum(jnp.where(mine, ipre, 0.0), axis=-1, keepdims=True)
    fgate = jnp.sum(jnp.where(mine, fpre, 0.0), axis=-1, keepdims=True)
    lforget = jnp.minimum(fgate, 0.0) - jnp.log1p(jnp.exp(-jnp.abs(fgate)))
    eye = lax.broadcasted_iota(jnp.int32, (R, R), 0) == lax.broadcasted_iota(jnp.int32, (R, R), 1)
    old_max = jnp.sum(jnp.where(eye, jnp.broadcast_to(mmax[...], (R, R)), 0.0), axis=-1, keepdims=True)
    held = lforget + old_max
    new_max = jnp.maximum(held, igate)
    keep = jnp.exp(held - new_max)
    admit = jnp.exp(igate - new_max)

    new_normalizer = keep * nrm[:, 0, :] + admit * key_vec
    q_cols = queries.T
    for b in range(R):
        num[b : b + 1, :] = jnp.sum(mem[b] * q_cols[:, b : b + 1], axis=0, keepdims=True)
    q_k = jnp.sum(queries * key_vec, axis=-1, keepdims=True)
    numerator = keep * num[...] + (admit * q_k) * values
    denominator = jnp.sum(queries * new_normalizer, axis=-1, keepdims=True)
    cell_out = numerator / jnp.maximum(jnp.abs(denominator), jnp.exp(-new_max))
    centered = cell_out - jnp.mean(cell_out, axis=-1, keepdims=True)
    head_var = jnp.mean(centered * centered, axis=-1, keepdims=True)
    mixed[t] = (jax.nn.sigmoid(outgate) * centered * lax.rsqrt(head_var + HEAD_EPS)).astype(BF16)

    m_copies = []
    for step in range(1, T):
        copy = send(mixed.at[t], mixed.at[t], m_send.at[step], m_recv.at[step], tp_peer(step))
        copy.start()
        m_copies.append(copy)

    newnrm[:, 0, :] = new_normalizer
    newmax[...] = jnp.sum(jnp.where(eye, jnp.broadcast_to(new_max, (R, R)), 0.0), axis=0, keepdims=True)
    k_cols = (admit * key_vec).T
    for b in range(R):
        newmem[b] = keep[b : b + 1, :] * mem[b] + k_cols[:, b : b + 1] * values[b : b + 1, :]
    outs = [
        pltpu.make_async_copy(newmem, newmem_hbm, out_sem.at[0]),
        pltpu.make_async_copy(newnrm, newnrm_hbm, out_sem.at[1]),
        pltpu.make_async_copy(newmax, newmax_hbm, out_sem.at[2]),
    ]
    for copy in outs:
        copy.start()

    loads["wout"].wait()
    loads["fgain"].wait()
    for copy in m_copies:
        copy.wait_recv()
    branch = jnp.zeros((R, CH), F32)
    for i in range(0, T, 2):
        pair = jnp.concatenate([mixed[i], mixed[i + 1]], axis=-1)
        branch += jnp.dot(pair, wout[i * HD : (i + 2) * HD, :], preferred_element_type=F32)
    resid = (tok[t].astype(F32) + branch).astype(BF16)
    rows[0, 0] = resid

    b_copies = {}
    for dy in near_first(Y):
        for dz in range(2):
            if dz or dy:
                copy = send(rows.at[0, 0], rows.at[dy, dz], b_send.at[dy, dz], b_recv.at[dy, dz], row_peer(dz, dy))
                copy.start()
                b_copies[dy, dz] = copy

    for i in range(2):
        for step in range(1, S):
            w_copies[i, step].wait_recv()
    up_and_gate = wgu[...].reshape(2 * GH, CH)
    gain = fgain[...]
    lane = lax.broadcasted_iota(jnp.int32, (2 * R, 2 * GH), 1)

    c_copies = []
    for dy in near_first(Y):
        for dz in range(2):
            if dz or dy:
                b_copies[dy, dz].wait_recv()
        block = rows[dy].reshape(2 * R, CH).astype(F32)
        part = transposed_rhs((block * gain).astype(BF16), up_and_gate)
        square = jnp.sum(block * block, axis=-1, keepdims=True)
        high = square.astype(BF16).astype(F32)
        part = jnp.where(lane == SHARD, high, jnp.where(lane == SHARD + 1, square - high, part)).astype(BF16)
        owner = (y - dy + Y) % Y
        csend[dy] = part

        @pl.when(owner == t)
        def _():
            cbuf[t] = part

        step = (owner - t + T) % T
        copy = send(csend.at[dy], cbuf.at[t], c_send.at[dy], c_recv.at[step], (kv, owner))

        @pl.when(owner != t)
        def _():
            copy.start()

        c_copies.append((owner, copy))

    for step in range(1, T):
        send(csend.at[0], cbuf.at[(t - step + T) % T], c_send.at[0], c_recv.at[step], tp_peer(step)).wait_recv()
    total = cbuf[0].astype(F32)
    for i in range(1, T):
        total += cbuf[i].astype(F32)
    square = jnp.sum(jnp.where((lane == SHARD) | (lane == SHARD + 1), total, 0.0), axis=-1, keepdims=True)
    ffn_scale = lax.rsqrt(square / width + EPS)
    gate_act = ffn_scale * total[:, :GH]
    up_act = ffn_scale * total[:, GH:]
    hid[t] = (jax.nn.silu(gate_act) * up_act).astype(BF16)
    d_copies = []
    for step in range(1, T):
        copy = send(hid.at[t], hid.at[t], d_send.at[step], d_recv.at[step], tp_peer(step))
        copy.start()
        d_copies.append(copy)

    for step in range(1, S):
        w_copies[2, step].wait_recv()
    down = wd[...].reshape(GH, CH)
    e_copies = {}
    total = rows[0, 0].astype(F32)
    for dy in near_first(Y):
        owner = (y - dy + Y) % Y
        step = (t - owner + T) % T
        copy = send(hid.at[t], hid.at[owner], d_send.at[0], d_recv.at[step], (kv, owner))

        @pl.when(owner != t)
        def _():
            copy.wait_recv()

        part = jnp.dot(hid[owner], down, preferred_element_type=F32)
        if dy == 0:
            total += part[:R]
        esend[dy] = part.astype(BF16).reshape(2, R, CH)
        for dz in range(2):
            if dz or dy:
                copy = send(esend.at[dy, dz], ebuf.at[dy, dz], e_send.at[dy, dz], e_recv.at[dy, dz], row_peer(dz, Y - dy))
                copy.start()
                e_copies[dy, dz] = copy

    for dy in near_first(Y):
        for dz in range(2):
            if dz or dy:
                e_copies[dy, dz].wait_recv()
                total += ebuf[dy, dz].astype(F32)
    outv[...] = total.astype(BF16)
    out = pltpu.make_async_copy(outv, res_hbm, out_sem.at[3])
    out.start()

    for copy in [*a_copies, *w_copies.values(), *m_copies, *b_copies.values(), *d_copies, *e_copies.values()]:
        copy.wait_send()
    for owner, copy in c_copies:

        @pl.when(owner != t)
        def _():
            copy.wait_send()

    for copy in outs:
        copy.wait()
    out.wait()


def per_device(Z, Y, T, *args):
    (tokens, norm_gain, w_query, w_key, w_value, w_outgate, w_input_gate, w_forget_gate,
     memory, normalizer, memory_max, w_output, ffn_gain, w_gate, w_up, w_down) = args
    R, CH = tokens.shape
    width, HD = w_query.shape
    heads = w_input_gate.shape[1]
    inner = w_output.shape[0]
    SHARD = w_down.shape[0]
    S = Z // 2
    PAD = -(-(SHARD + 2) // 32) * 32
    GH = S * PAD
    any_spec = pl.BlockSpec(memory_space=pl.ANY)
    dma = pltpu.SemaphoreType.DMA
    outs = (
        jax.ShapeDtypeStruct((R, CH), BF16),
        jax.ShapeDtypeStruct((R, HD, HD), F32),
        jax.ShapeDtypeStruct((R, 1, HD), F32),
        jax.ShapeDtypeStruct((1, R), F32),
    )
    result, new_memory, new_normalizer, new_max = pl.pallas_call(
        functools.partial(kernel, Z, Y, T, S, SHARD, PAD),
        name="layer",
        out_shape=outs,
        in_specs=[any_spec] * 16,
        out_specs=(any_spec,) * 4,
        scratch_shapes=[
            pltpu.VMEM((T, R, CH), BF16),
            pltpu.VMEM((1, width), F32),
            pltpu.VMEM((width, 4 * HD), BF16),
            pltpu.VMEM((2, heads, width), BF16),
            pltpu.VMEM((R, HD, HD), F32),
            pltpu.VMEM((R, 1, HD), F32),
            pltpu.VMEM((1, R), F32),
            pltpu.VMEM((inner, CH), BF16),
            pltpu.VMEM((1, CH), F32),
            pltpu.VMEM((2, S, PAD, CH), BF16),
            pltpu.VMEM((S, PAD, CH), BF16),
            pltpu.VMEM((R, HD, HD), F32),
            pltpu.VMEM((R, 1, HD), F32),
            pltpu.VMEM((1, R), F32),
            pltpu.VMEM((R, HD), F32),
            pltpu.VMEM((T, R, HD), BF16),
            pltpu.VMEM((Y, 2, R, CH), BF16),
            pltpu.VMEM((Y, 2 * R, 2 * GH), BF16),
            pltpu.VMEM((T, 2 * R, 2 * GH), BF16),
            pltpu.VMEM((T, 2 * R, GH), BF16),
            pltpu.VMEM((Y, 2, R, CH), BF16),
            pltpu.VMEM((Y, 2, R, CH), BF16),
            pltpu.VMEM((R, CH), BF16),
            dma((16,)), dma((4,)), dma((T,)), dma((T,)), dma((3, S)), dma((3, S)), dma((T,)), dma((T,)),
            dma((Y, 2)), dma((Y, 2)), dma((Y,)), dma((T,)), dma((T,)), dma((T,)), dma((Y, 2)), dma((Y, 2)),
        ],
        compiler_params=pltpu.CompilerParams(collective_id=0, has_side_effects=True),
    )(
        tokens, norm_gain.reshape(1, width), w_query, w_key, w_value, w_outgate,
        w_input_gate.T, w_forget_gate.T, memory.reshape(R, HD, HD), normalizer, memory_max.T,
        w_output, ffn_gain.reshape(1, CH), w_gate.T, w_up.T, w_down,
    )
    return result, new_memory.reshape(R, 1, HD, HD), new_normalizer, new_max.T


def solution(mesh):
    placed = (
        P("kv", "tp"), P(),
        P(None, "tp"), P(None, "tp"), P(None, "tp"), P(None, "tp"),
        P(), P(),
        P("kv", "tp", None, None), P("kv", "tp", None), P("kv", "tp"),
        P(None, "tp"), P("tp"), P("tp", "kv"), P("tp", "kv"), P("kv", "tp"),
    )
    T = mesh.shape["tp"]
    Z, Y = mesh.shape["kv"] // T, T
    return jax.shard_map(
        functools.partial(per_device, Z, Y, T),
        mesh=mesh,
        in_specs=placed,
        out_specs=(P("kv", "tp"), P("kv", "tp", None, None), P("kv", "tp", None), P("kv", "tp")),
        check_vma=False,
    )
```

```python
import functools

import jax
import jax.numpy as jnp
from jax import lax
from jax.experimental import pallas as pl
from jax.experimental.pallas import tpu as pltpu
from jax.sharding import PartitionSpec as P

EPS = 1e-06
HEAD_EPS = 1e-05
F32 = jnp.float32
BF16 = jnp.bfloat16
MESH = pl.DeviceIdType.MESH


def transposed_rhs(a, b):
    return lax.dot_general(a, b, (((1,), (1,)), ((), ())), preferred_element_type=F32)


def near_first(n):
    order = [0]
    for step in range(1, n // 2 + 1):
        order += [step] if step == n - step else [step, n - step]
    return order


def kernel(
    Z, Y, T, S, SHARD, PAD,
    tok_hbm, ngain_hbm, wq_hbm, wk_hbm, wv_hbm, wo_hbm, wig_hbm, wfg_hbm,
    mem_hbm, nrm_hbm, mmax_hbm, wout_hbm, fgain_hbm, wg_hbm, wu_hbm, wd_hbm,
    outv, newmem, newnrm, newmax,
    tok, ngain, wproj, wgates, mem, nrm, mmax, wout, fgain, mix,
    num, mixed, rows, csend, cbuf, hid, esend, ebuf,
    load_sem, up_sem, ready, a_send, a_recv, w_send, w_recv, m_send, m_recv, b_send, b_recv,
    c_send, c_recv, d_send, d_recv, e_send, e_recv,
):
    kv = lax.axis_index("kv")
    t = lax.axis_index("tp")
    z, y = kv // Y, kv % Y
    par = z % 2
    base = z - par
    R, CH = tok.shape[1], tok.shape[2]
    HD = mem.shape[1]
    width = T * CH
    GH = S * PAD

    def tp_peer(step):
        return (kv, (t + step) % T)

    def row_peer(dz, dy):
        return ((base + (par + dz) % 2) * Y + (y + dy) % Y, t)

    def column(other):
        return (other * Y + y, t)

    for s in range(S):
        for i in range(3):
            mix[i, s, SHARD:PAD, :] = jnp.zeros((PAD - SHARD, CH), BF16)
    loads = {}

    def load(name, src, dst):
        copy = pltpu.make_async_copy(src, dst, load_sem.at[len(loads)])
        copy.start()
        loads[name] = copy

    load("tok", tok_hbm, tok.at[t])
    load("wg", wg_hbm, mix.at[0, 0, pl.ds(0, SHARD)])
    load("wu", wu_hbm, mix.at[1, 0, pl.ds(0, SHARD)])
    load("wd", wd_hbm, mix.at[2, 0, pl.ds(0, SHARD)])
    load("ngain", ngain_hbm, ngain)
    for i, w in enumerate((wq_hbm, wk_hbm, wv_hbm, wo_hbm)):
        load(f"w{i}", w, wproj.at[:, pl.ds(i * HD, HD)])
    load("wig", wig_hbm, wgates.at[0])
    load("wfg", wfg_hbm, wgates.at[1])
    load("mmax", mmax_hbm, mmax)
    load("nrm", nrm_hbm, nrm)
    load("mem", mem_hbm, mem)
    load("wout", wout_hbm, wout)
    load("fgain", fgain_hbm, fgain)

    barrier = pltpu.get_barrier_semaphore()
    peers = [tp_peer(step) for step in range(1, T)]
    peers += [row_peer(dz, dy) for dy in near_first(Y) for dz in range(2) if dz or dy]
    for peer in peers:
        pl.semaphore_signal(barrier, inc=1, device_id=peer, device_id_type=MESH)
    beside = z - 1 + 2 * par
    inner = (beside >= 0) & (beside < Z)

    @pl.when(inner)
    def _():
        pl.semaphore_signal(barrier, inc=1, device_id=column(beside), device_id_type=MESH)

    loads["tok"].wait()

    @pl.when(inner)
    def _():
        pl.semaphore_wait(barrier, len(peers) + 1)

    @pl.when(jnp.logical_not(inner))
    def _():
        pl.semaphore_wait(barrier, len(peers))

    def send(src, dst, ssem, rsem, peer):
        copy = pltpu.make_async_remote_copy(
            src_ref=src, dst_ref=dst, send_sem=ssem, recv_sem=rsem,
            device_id=peer, device_id_type=MESH,
        )
        return copy

    a_copies = []
    for step in range(1, T):
        copy = send(tok.at[t], tok.at[t], a_send.at[step], a_recv.at[step], tp_peer(step))
        copy.start()
        a_copies.append(copy)

    @pl.when(z > 0)
    def _():
        pl.semaphore_wait(up_sem, 1)

    @pl.when(z < Z - 1)
    def _():
        pl.semaphore_signal(up_sem, inc=1, device_id=column(z + 1), device_id_type=MESH)

    for step in range(1, S):

        @pl.when(z >= 2 * step)
        def _():
            pl.semaphore_signal(ready.at[step], inc=1, device_id=column(z - 2 * step), device_id_type=MESH)

    def shard_copy(piece, above, step):
        part = pl.ds(0, 2) if piece == 0 else pl.ds(2, 1)
        slot = S - step if above else step
        other = z + 2 * step if above else z - 2 * step
        return send(
            mix.at[part, 0, pl.ds(0, SHARD)], mix.at[part, slot, pl.ds(0, SHARD)],
            w_send.at[piece, above, step], w_recv.at[piece, slot], column(other),
        )

    def shard_exists(above, step):
        return z + 2 * step < Z if above else z >= 2 * step

    def to_below(piece):
        for step in range(1, S):

            @pl.when(shard_exists(0, step))
            def _():
                shard_copy(piece, 0, step).start()

    def to_above(steps):
        for step in steps:

            @pl.when(shard_exists(1, step))
            def _():
                pl.semaphore_wait(ready.at[step], 1)
                shard_copy(0, 1, step).start()
                shard_copy(1, 1, step).start()

    def shard_arrives(piece):
        for slot in range(1, S):
            shard_copy(piece, 0, slot).wait_recv()

    loads["wg"].wait()
    loads["wu"].wait()
    loads["wd"].wait()
    to_below(0)
    to_below(1)

    for name in ("ngain", "w0", "w1", "w2", "w3", "wig", "wfg", "mmax", "nrm", "mem"):
        loads[name].wait()
    for copy in a_copies:
        copy.wait_recv()

    blocks = [tok[i].astype(F32) for i in range(T)]
    square = sum(jnp.sum(b * b, axis=-1, keepdims=True) for b in blocks)
    row_scale = lax.rsqrt(square / width + EPS)
    proj = jnp.zeros((R, 4 * HD), F32)
    ipre = jnp.zeros((R, wgates.shape[1]), F32)
    fpre = jnp.zeros((R, wgates.shape[1]), F32)
    for i in range(T):
        cols = slice(i * CH, (i + 1) * CH)
        normed = (blocks[i] * row_scale * ngain[:, cols]).astype(BF16)
        proj += jnp.dot(normed, wproj[cols, :], preferred_element_type=F32)
        ipre += transposed_rhs(normed, wgates[0, :, cols])
        fpre += transposed_rhs(normed, wgates[1, :, cols])
    queries = proj[:, :HD] * HD ** (-0.5)
    key_vec = proj[:, HD : 2 * HD]
    values = proj[:, 2 * HD : 3 * HD]
    outgate = proj[:, 3 * HD :]
    mine = lax.broadcasted_iota(jnp.int32, ipre.shape, 1) == t
    igate = jnp.sum(jnp.where(mine, ipre, 0.0), axis=-1, keepdims=True)
    fgate = jnp.sum(jnp.where(mine, fpre, 0.0), axis=-1, keepdims=True)
    lforget = jnp.minimum(fgate, 0.0) - jnp.log1p(jnp.exp(-jnp.abs(fgate)))
    eye = lax.broadcasted_iota(jnp.int32, (R, R), 0) == lax.broadcasted_iota(jnp.int32, (R, R), 1)
    old_max = jnp.sum(jnp.where(eye, jnp.broadcast_to(mmax[...], (R, R)), 0.0), axis=-1, keepdims=True)
    held = lforget + old_max
    new_max = jnp.maximum(held, igate)
    keep = jnp.exp(held - new_max)
    admit = jnp.exp(igate - new_max)

    new_normalizer = keep * nrm[:, 0, :] + admit * key_vec
    q_cols = queries.T
    for b in range(R):
        num[b : b + 1, :] = jnp.sum(mem[b] * q_cols[:, b : b + 1], axis=0, keepdims=True)
    q_k = jnp.sum(queries * key_vec, axis=-1, keepdims=True)
    numerator = keep * num[...] + (admit * q_k) * values
    denominator = jnp.sum(queries * new_normalizer, axis=-1, keepdims=True)
    cell_out = numerator / jnp.maximum(jnp.abs(denominator), jnp.exp(-new_max))
    centered = cell_out - jnp.mean(cell_out, axis=-1, keepdims=True)
    head_var = jnp.mean(centered * centered, axis=-1, keepdims=True)
    mixed[t] = (jax.nn.sigmoid(outgate) * centered * lax.rsqrt(head_var + HEAD_EPS)).astype(BF16)

    m_copies = []
    for step in range(1, T):
        copy = send(mixed.at[t], mixed.at[t], m_send.at[step], m_recv.at[step], tp_peer(step))
        copy.start()
        m_copies.append(copy)

    to_above(range(1, 2))
    newnrm[:, 0, :] = new_normalizer
    newmax[...] = jnp.sum(jnp.where(eye, jnp.broadcast_to(new_max, (R, R)), 0.0), axis=0, keepdims=True)
    k_cols = (admit * key_vec).T
    for b in range(R):
        newmem[b] = keep[b : b + 1, :] * mem[b] + k_cols[:, b : b + 1] * values[b : b + 1, :]

    loads["wout"].wait()
    loads["fgain"].wait()
    for copy in m_copies:
        copy.wait_recv()
    branch = jnp.zeros((R, CH), F32)
    for i in range(0, T, 2):
        pair = jnp.concatenate([mixed[i], mixed[i + 1]], axis=-1)
        branch += jnp.dot(pair, wout[i * HD : (i + 2) * HD, :], preferred_element_type=F32)
    resid = (tok[t].astype(F32) + branch).astype(BF16)
    rows[0, 0] = resid

    b_copies = {}
    for dy in near_first(Y):
        for dz in range(2):
            if dz or dy:
                copy = send(rows.at[0, 0], rows.at[dy, dz], b_send.at[dy, dz], b_recv.at[dy, dz], row_peer(dz, dy))
                copy.start()
                b_copies[dy, dz] = copy

    to_above(range(2, S))
    shard_arrives(0)
    up_and_gate = mix[0:2].reshape(2 * GH, CH)
    gain = fgain[...]
    lane = lax.broadcasted_iota(jnp.int32, (2 * R, 2 * GH), 1)

    c_copies = []
    for dy in near_first(Y):
        for dz in range(2):
            if dz or dy:
                b_copies[dy, dz].wait_recv()
        block = rows[dy].reshape(2 * R, CH).astype(F32)
        part = transposed_rhs((block * gain).astype(BF16), up_and_gate)
        square = jnp.sum(block * block, axis=-1, keepdims=True)
        high = square.astype(BF16).astype(F32)
        part = jnp.where(lane == SHARD, high, jnp.where(lane == SHARD + 1, square - high, part)).astype(BF16)
        owner = (y - dy + Y) % Y
        csend[dy] = part

        @pl.when(owner == t)
        def _():
            cbuf[t] = part

        step = (owner - t + T) % T
        copy = send(csend.at[dy], cbuf.at[t], c_send.at[dy], c_recv.at[step], (kv, owner))

        @pl.when(owner != t)
        def _():
            copy.start()

        c_copies.append((owner, copy))

    for step in range(1, T):
        send(csend.at[0], cbuf.at[(t - step + T) % T], c_send.at[0], c_recv.at[step], tp_peer(step)).wait_recv()
    total = cbuf[0].astype(F32)
    for i in range(1, T):
        total += cbuf[i].astype(F32)
    square = jnp.sum(jnp.where((lane == SHARD) | (lane == SHARD + 1), total, 0.0), axis=-1, keepdims=True)
    ffn_scale = lax.rsqrt(square / width + EPS)
    gate_act = ffn_scale * total[:, :GH]
    up_act = ffn_scale * total[:, GH:]
    hid[t] = (jax.nn.silu(gate_act) * up_act).astype(BF16)
    d_copies = []
    for step in range(1, T):
        copy = send(hid.at[t], hid.at[t], d_send.at[step], d_recv.at[step], tp_peer(step))
        copy.start()
        d_copies.append(copy)

    shard_arrives(1)
    down = mix[2].reshape(GH, CH)
    e_copies = {}
    total = rows[0, 0].astype(F32)
    for dy in near_first(Y):
        owner = (y - dy + Y) % Y
        step = (t - owner + T) % T
        copy = send(hid.at[t], hid.at[owner], d_send.at[0], d_recv.at[step], (kv, owner))

        @pl.when(owner != t)
        def _():
            copy.wait_recv()

        part = jnp.dot(hid[owner], down, preferred_element_type=F32)
        if dy == 0:
            total += part[:R]
        esend[dy] = part.astype(BF16).reshape(2, R, CH)
        for dz in range(2):
            if dz or dy:
                copy = send(esend.at[dy, dz], ebuf.at[dy, dz], e_send.at[dy, dz], e_recv.at[dy, dz], row_peer(dz, Y - dy))
                copy.start()
                e_copies[dy, dz] = copy

    for dy in near_first(Y):
        for dz in range(2):
            if dz or dy:
                e_copies[dy, dz].wait_recv()
                total += ebuf[dy, dz].astype(F32)
    outv[...] = total.astype(BF16)
    for copy in [*a_copies, *m_copies, *b_copies.values(), *d_copies, *e_copies.values()]:
        copy.wait_send()
    for owner, copy in c_copies:

        @pl.when(owner != t)
        def _():
            copy.wait_send()

    for above in range(2):
        for step in range(1, S):

            @pl.when(shard_exists(above, step))
            def _():
                shard_copy(0, above, step).wait_send()
                shard_copy(1, above, step).wait_send()


def store(*refs):
    sem = refs[-1]
    copies = [pltpu.make_async_copy(refs[i], refs[4 + i], sem.at[i]) for i in range(4)]
    for copy in copies:
        copy.start()
    for copy in copies:
        copy.wait()


def per_device(Z, Y, T, *args):
    (tokens, norm_gain, w_query, w_key, w_value, w_outgate, w_input_gate, w_forget_gate,
     memory, normalizer, memory_max, w_output, ffn_gain, w_gate, w_up, w_down) = args
    R, CH = tokens.shape
    width, HD = w_query.shape
    heads = w_input_gate.shape[1]
    inner = w_output.shape[0]
    SHARD = w_down.shape[0]
    S = Z // 2
    PAD = -(-(SHARD + 2) // 32) * 32
    GH = S * PAD
    any_spec = pl.BlockSpec(memory_space=pl.ANY)
    dma = pltpu.SemaphoreType.DMA
    outs = (
        jax.ShapeDtypeStruct((R, CH), BF16),
        jax.ShapeDtypeStruct((R, HD, HD), F32),
        jax.ShapeDtypeStruct((R, 1, HD), F32),
        jax.ShapeDtypeStruct((1, R), F32),
    )
    held = pl.pallas_call(
        functools.partial(kernel, Z, Y, T, S, SHARD, PAD),
        name="layer",
        out_shape=tuple(pltpu.VMEM(o.shape, o.dtype) for o in outs),
        in_specs=[any_spec] * 16,
        out_specs=(pl.BlockSpec(memory_space=pltpu.VMEM),) * 4,
        scratch_shapes=[
            pltpu.VMEM((T, R, CH), BF16),
            pltpu.VMEM((1, width), F32),
            pltpu.VMEM((width, 4 * HD), BF16),
            pltpu.VMEM((2, heads, width), BF16),
            pltpu.VMEM((R, HD, HD), F32),
            pltpu.VMEM((R, 1, HD), F32),
            pltpu.VMEM((1, R), F32),
            pltpu.VMEM((inner, CH), BF16),
            pltpu.VMEM((1, CH), F32),
            pltpu.VMEM((3, S, PAD, CH), BF16),
            pltpu.VMEM((R, HD), F32),
            pltpu.VMEM((T, R, HD), BF16),
            pltpu.VMEM((Y, 2, R, CH), BF16),
            pltpu.VMEM((Y, 2 * R, 2 * GH), BF16),
            pltpu.VMEM((T, 2 * R, 2 * GH), BF16),
            pltpu.VMEM((T, 2 * R, GH), BF16),
            pltpu.VMEM((Y, 2, R, CH), BF16),
            pltpu.VMEM((Y, 2, R, CH), BF16),
            dma((16,)), pltpu.SemaphoreType.REGULAR, pltpu.SemaphoreType.REGULAR((S,)),
            dma((T,)), dma((T,)), dma((2, 2, S)), dma((2, S)), dma((T,)), dma((T,)),
            dma((Y, 2)), dma((Y, 2)), dma((Y,)), dma((T,)), dma((T,)), dma((T,)), dma((Y, 2)), dma((Y, 2)),
        ],
        compiler_params=pltpu.CompilerParams(collective_id=0, has_side_effects=True),
    )(
        tokens, norm_gain.reshape(1, width), w_query, w_key, w_value, w_outgate,
        w_input_gate.T, w_forget_gate.T, memory.reshape(R, HD, HD), normalizer, memory_max.T,
        w_output, ffn_gain.reshape(1, CH), w_gate.T, w_up.T, w_down,
    )
    result, new_memory, new_normalizer, new_max = pl.pallas_call(
        store,
        name="store",
        out_shape=outs,
        in_specs=[pl.BlockSpec(memory_space=pltpu.VMEM)] * 4,
        out_specs=(any_spec,) * 4,
        scratch_shapes=[dma((4,))],
    )(*[pltpu.with_memory_space_constraint(h, pltpu.VMEM) for h in held])
    return result, new_memory.reshape(R, 1, HD, HD), new_normalizer, new_max.T


def solution(mesh):
    placed = (
        P("kv", "tp"), P(),
        P(None, "tp"), P(None, "tp"), P(None, "tp"), P(None, "tp"),
        P(), P(),
        P("kv", "tp", None, None), P("kv", "tp", None), P("kv", "tp"),
        P(None, "tp"), P("tp"), P("tp", "kv"), P("tp", "kv"), P("kv", "tp"),
    )
    T = mesh.shape["tp"]
    Z, Y = mesh.shape["kv"] // T, T
    return jax.shard_map(
        functools.partial(per_device, Z, Y, T),
        mesh=mesh,
        in_specs=placed,
        out_specs=(P("kv", "tp"), P("kv", "tp", None, None), P("kv", "tp", None), P("kv", "tp")),
        check_vma=False,
    )
```

```python
import functools

import jax
import jax.numpy as jnp
from jax import lax
from jax.experimental import pallas as pl
from jax.experimental.pallas import tpu as pltpu
from jax.sharding import PartitionSpec as P

EPS = 1e-06
HEAD_EPS = 1e-05
F32 = jnp.float32
BF16 = jnp.bfloat16
MESH = pl.DeviceIdType.MESH


def transposed_rhs(a, b):
    return lax.dot_general(a, b, (((1,), (1,)), ((), ())), preferred_element_type=F32)


def near_first(n):
    order = [0]
    for step in range(1, n // 2 + 1):
        order += [step] if step == n - step else [step, n - step]
    return order


def kernel(
    Z, Y, T, S, SHARD, PAD,
    tok_hbm, ngain_hbm, wq_hbm, wk_hbm, wv_hbm, wo_hbm, wig_hbm, wfg_hbm,
    mem_hbm, nrm_hbm, mmax_hbm, wout_hbm, fgain_hbm, wg_hbm, wu_hbm, wd_hbm,
    outv, newmem, newnrm, newmax,
    tok, ngain, wproj, wgates, mem, nrm, mmax, wout, fgain, mix,
    num, mixed, resid_buf, rows, csend, cbuf, hid, esend, ebuf,
    load_sem, up_sem, ready, a_send, a_recv, w_send, w_recv, r_send, r_recv, p_send, p_recv, g_send, g_recv,
    m_send, m_recv, b_send, b_recv, c_send, c_recv, d_send, d_recv, e_send, e_recv,
):
    kv = lax.axis_index("kv")
    t = lax.axis_index("tp")
    z, y = kv // Y, kv % Y
    x, core = t // 2, t % 2
    par = z % 2
    base = z - par
    R, CH = tok.shape[1], tok.shape[2]
    HD = mem.shape[1]
    X, K = T // 2, Y // 2
    width = T * CH
    GH = S * PAD
    odd = (y + core) % 2
    home = y % 2
    at_home = core == home
    middle = (z >= 2) & (z < Z - 2)
    order = [k // 2 if k % 2 == 0 else K - 1 - k // 2 for k in range(K)]

    def tp_peer(step):
        return (kv, (t + step) % T)

    def row_peer(dz, dy, side):
        return ((base + (par + dz) % 2) * Y + (y + dy) % Y, 2 * x + side)

    def column(other):
        return (other * Y + y, t)

    above, below = (z + 2) % Z, (z + Z - 2) % Z
    partner = (kv, 2 * x + 1 - core)

    def send(src, dst, ssem, rsem, peer):
        return pltpu.make_async_remote_copy(
            src_ref=src, dst_ref=dst, send_sem=ssem, recv_sem=rsem,
            device_id=peer, device_id_type=MESH,
        )

    loads = {}

    def load(name, src, dst):
        copy = pltpu.make_async_copy(src, dst, load_sem.at[len(loads)])
        copy.start()
        loads[name] = copy

    for side in range(2):
        for s in range(S):
            for i in range(3):
                mix[side, i, s, SHARD:PAD, :] = jnp.zeros((PAD - SHARD, CH), BF16)
    load("tok", tok_hbm, tok.at[t])
    load("wg", wg_hbm, mix.at[core, 0, 0, pl.ds(0, SHARD)])
    load("wu", wu_hbm, mix.at[core, 1, 0, pl.ds(0, SHARD)])
    load("wd", wd_hbm, mix.at[core, 2, 0, pl.ds(0, SHARD)])
    load("ngain", ngain_hbm, ngain)
    for i, w in enumerate((wq_hbm, wk_hbm, wv_hbm, wo_hbm)):
        load(f"w{i}", w, wproj.at[:, pl.ds(i * HD, HD)])
    load("wig", wig_hbm, wgates.at[0])
    load("wfg", wfg_hbm, wgates.at[1])
    load("mmax", mmax_hbm, mmax)
    load("nrm", nrm_hbm, nrm)
    load("mem", mem_hbm, mem)
    load("wout", wout_hbm, wout)
    load("fgain", fgain_hbm, fgain.at[core])

    barrier = pltpu.get_barrier_semaphore()
    peers = [tp_peer(step) for step in range(1, T)]
    for dy in near_first(Y):
        for dz in range(2):
            if dz or dy:
                peers += [row_peer(dz, dy, 0), row_peer(dz, dy, 1)]
    for peer in peers:
        pl.semaphore_signal(barrier, inc=1, device_id=peer, device_id_type=MESH)
    beside = z - 1 + 2 * par
    inner = (beside >= 0) & (beside < Z)

    @pl.when(inner)
    def _():
        pl.semaphore_signal(barrier, inc=1, device_id=column(beside), device_id_type=MESH)

    loads["tok"].wait()

    @pl.when(inner)
    def _():
        pl.semaphore_wait(barrier, len(peers) + 1)

    @pl.when(jnp.logical_not(inner))
    def _():
        pl.semaphore_wait(barrier, len(peers))

    a_copies = []
    for step in range(1, T):
        copy = send(tok.at[t], tok.at[t], a_send.at[step], a_recv.at[step], tp_peer(step))
        copy.start()
        a_copies.append(copy)

    @pl.when(z > 0)
    def _():
        pl.semaphore_wait(up_sem, 1)

    @pl.when(z < Z - 1)
    def _():
        pl.semaphore_signal(up_sem, inc=1, device_id=column(z + 1), device_id_type=MESH)

    @pl.when(z >= 2)
    def _():
        pl.semaphore_signal(ready.at[0], inc=1, device_id=column(below), device_id_type=MESH)

    @pl.when(z >= Z - 2)
    def _():
        pl.semaphore_signal(ready.at[1], inc=1, device_id=column(above), device_id_type=MESH)

    def piece_at(piece, slot):
        part = pl.ds(0, 2) if piece == 0 else pl.ds(2, 1)
        return mix.at[core, part, slot, pl.ds(0, SHARD)]

    def direct(piece, up):
        slot = S - 1 if up else 1
        return send(piece_at(piece, 0), piece_at(piece, slot), w_send.at[piece, up], w_recv.at[piece, slot],
                    column(above if up else below))

    def relay(piece, up):
        return send(piece_at(piece, S - 1 if up else 1), piece_at(piece, 2), r_send.at[piece, up], r_recv.at[piece],
                    column(above if up else below))

    def forward(piece, slot):
        return send(piece_at(piece, slot), piece_at(piece, slot), p_send.at[piece, slot], p_recv.at[piece, slot], partner)

    def direct_both(up):
        direct(0, up).start()
        direct(1, up).start()

    def pass_on(piece, relayed):
        for up in range(2):
            slot = S - 1 if up else 1
            direct(piece, 1 if slot == S - 1 else 0).wait_recv()
            if relayed:
                relay(piece, up).start()
            forward(piece, slot).start()

    loads["wg"].wait()
    loads["wu"].wait()
    loads["wd"].wait()

    @pl.when(z >= 2)
    def _():
        direct_both(0)

    @pl.when(z >= Z - 2)
    def _():
        direct_both(1)

    forward(0, 0).start()
    forward(1, 0).start()
    loads["fgain"].wait()
    gain_copy = send(fgain.at[core], fgain.at[core], g_send, g_recv, partner)
    gain_copy.start()

    for name in ("ngain", "w0", "w1", "w2", "w3", "wig", "wfg", "mmax", "nrm", "mem"):
        loads[name].wait()
    for copy in a_copies:
        copy.wait_recv()

    @pl.when(z < Z - 2)
    def _():
        pl.semaphore_wait(ready.at[0], 1)
        direct_both(1)

    blocks = [tok[i].astype(F32) for i in range(T)]
    square = sum(jnp.sum(b * b, axis=-1, keepdims=True) for b in blocks)
    row_scale = lax.rsqrt(square / width + EPS)
    proj = jnp.zeros((R, 4 * HD), F32)
    ipre = jnp.zeros((R, wgates.shape[1]), F32)
    fpre = jnp.zeros((R, wgates.shape[1]), F32)
    for i in range(T):
        cols = slice(i * CH, (i + 1) * CH)
        normed = (blocks[i] * row_scale * ngain[:, cols]).astype(BF16)
        proj += jnp.dot(normed, wproj[cols, :], preferred_element_type=F32)
        ipre += transposed_rhs(normed, wgates[0, :, cols])
        fpre += transposed_rhs(normed, wgates[1, :, cols])
    queries = proj[:, :HD] * HD ** (-0.5)
    key_vec = proj[:, HD : 2 * HD]
    values = proj[:, 2 * HD : 3 * HD]
    outgate = proj[:, 3 * HD :]
    mine = lax.broadcasted_iota(jnp.int32, ipre.shape, 1) == t
    igate = jnp.sum(jnp.where(mine, ipre, 0.0), axis=-1, keepdims=True)
    fgate = jnp.sum(jnp.where(mine, fpre, 0.0), axis=-1, keepdims=True)
    lforget = jnp.minimum(fgate, 0.0) - jnp.log1p(jnp.exp(-jnp.abs(fgate)))
    eye = lax.broadcasted_iota(jnp.int32, (R, R), 0) == lax.broadcasted_iota(jnp.int32, (R, R), 1)
    old_max = jnp.sum(jnp.where(eye, jnp.broadcast_to(mmax[...], (R, R)), 0.0), axis=-1, keepdims=True)
    held = lforget + old_max
    new_max = jnp.maximum(held, igate)
    keep = jnp.exp(held - new_max)
    admit = jnp.exp(igate - new_max)

    new_normalizer = keep * nrm[:, 0, :] + admit * key_vec
    q_cols = queries.T
    for b in range(R):
        num[b : b + 1, :] = jnp.sum(mem[b] * q_cols[:, b : b + 1], axis=0, keepdims=True)
    q_k = jnp.sum(queries * key_vec, axis=-1, keepdims=True)
    numerator = keep * num[...] + (admit * q_k) * values
    denominator = jnp.sum(queries * new_normalizer, axis=-1, keepdims=True)
    cell_out = numerator / jnp.maximum(jnp.abs(denominator), jnp.exp(-new_max))
    centered = cell_out - jnp.mean(cell_out, axis=-1, keepdims=True)
    head_var = jnp.mean(centered * centered, axis=-1, keepdims=True)
    mixed[t] = (jax.nn.sigmoid(outgate) * centered * lax.rsqrt(head_var + HEAD_EPS)).astype(BF16)

    m_copies = []
    for step in range(1, T):
        copy = send(mixed.at[t], mixed.at[t], m_send.at[step], m_recv.at[step], tp_peer(step))
        copy.start()
        m_copies.append(copy)

    newnrm[:, 0, :] = new_normalizer
    newmax[...] = jnp.sum(jnp.where(eye, jnp.broadcast_to(new_max, (R, R)), 0.0), axis=0, keepdims=True)
    k_cols = (admit * key_vec).T
    for b in range(R):
        newmem[b] = keep[b : b + 1, :] * mem[b] + k_cols[:, b : b + 1] * values[b : b + 1, :]

    @pl.when(middle)
    def _():
        pass_on(0, True)

    loads["wout"].wait()
    for copy in m_copies:
        copy.wait_recv()
    branch = jnp.zeros((R, CH), F32)
    for i in range(0, T, 2):
        pair = jnp.concatenate([mixed[i], mixed[i + 1]], axis=-1)
        branch += jnp.dot(pair, wout[i * HD : (i + 2) * HD, :], preferred_element_type=F32)
    resid = (tok[t].astype(F32) + branch).astype(BF16)
    resid_buf[...] = resid

    def row_copy(dy, dz):
        return send(resid_buf, rows.at[dy // 2, core, dz], b_send.at[dy, dz], b_recv.at[dy // 2, core, dz],
                    row_peer(dz, dy, home))

    for dy in near_first(Y):
        for dz in range(2):
            if dz or dy:
                row_copy(dy, dz).start()

    @pl.when(at_home)
    def _():
        rows[0, core, 0] = resid

    @pl.when(jnp.logical_not(at_home))
    def _():
        row_copy(0, 0).start()

    @pl.when(z < 2)
    def _():
        pl.semaphore_wait(ready.at[1], 1)
        direct_both(0)

    @pl.when(jnp.logical_not(middle))
    def _():
        pass_on(0, False)

    relay(0, 0).wait_recv()
    forward(0, 2).start()

    @pl.when(middle)
    def _():
        pass_on(1, True)

    @pl.when(jnp.logical_not(middle))
    def _():
        pass_on(1, False)

    for slot in range(S):
        forward(0, slot).wait_recv()

    up_and_gate = [mix[side, 0:2].reshape(2 * GH, CH) for side in range(2)]
    gain_copy.wait_recv()
    gain = [fgain[side] for side in range(2)]
    lane = lax.broadcasted_iota(jnp.int32, (2 * R, 2 * GH), 1)
    c_copies = []
    group = max(1, K // 2)
    for first in range(0, K, group):
        ks = order[first : first + group]
        for k in ks:
            for side in range(2):
                for dz in range(2):
                    copy = send(resid_buf, rows.at[k, side, dz], b_send.at[0, 0], b_recv.at[k, side, dz], partner)
                    if k or dz:
                        copy.wait_recv()
                    else:

                        @pl.when(jnp.logical_not(at_home & (core == side)))
                        def _():
                            copy.wait_recv()

        total = 0.0
        square = 0.0
        for side in range(2):
            block = jnp.concatenate([rows[k, side].reshape(2 * R, CH) for k in ks], axis=0).astype(F32)
            square += jnp.sum(block * block, axis=-1, keepdims=True)
            total += transposed_rhs((block * gain[side]).astype(BF16), up_and_gate[side])
        for i, k in enumerate(ks):
            part = total[i * 2 * R : (i + 1) * 2 * R]
            sq = square[i * 2 * R : (i + 1) * 2 * R]
            high = sq.astype(BF16).astype(F32)
            part = jnp.where(lane == SHARD, high, jnp.where(lane == SHARD + 1, sq - high, part)).astype(BF16)
            owner = (y - 2 * k - odd + 2 * Y) % Y
            csend[k] = part

            @pl.when(owner == t)
            def _():
                cbuf[x] = part

            copy = send(csend.at[k], cbuf.at[x], c_send.at[k], c_recv.at[x], (kv, owner))

            @pl.when(owner != t)
            def _():
                copy.start()

            c_copies.append((owner, copy))

    for step in range(1, X):
        sender = (x + step) % X
        send(csend.at[0], cbuf.at[sender], c_send.at[0], c_recv.at[sender], (kv, 2 * sender + core)).wait_recv()
    total = cbuf[0].astype(F32)
    for i in range(1, X):
        total += cbuf[i].astype(F32)
    square = jnp.sum(jnp.where((lane == SHARD) | (lane == SHARD + 1), total, 0.0), axis=-1, keepdims=True)
    ffn_scale = lax.rsqrt(square / width + EPS)
    gate_act = ffn_scale * total[:, :GH]
    up_act = ffn_scale * total[:, GH:]
    hid[x] = (jax.nn.silu(gate_act) * up_act).astype(BF16)
    d_copies = []
    for step in range(1, X):
        copy = send(hid.at[x], hid.at[x], d_send.at[step], d_recv.at[x], (kv, 2 * ((x + step) % X) + core))
        copy.start()
        d_copies.append(copy)

    relay(1, 0).wait_recv()
    forward(1, 2).start()
    for slot in range(S):
        forward(1, slot).wait_recv()
    down = [mix[side, 2].reshape(GH, CH) for side in range(2)]
    e_copies = []
    for k in order:
        owner = (y - 2 * k - odd + 2 * Y) % Y
        source = owner // 2
        copy = send(hid.at[source], hid.at[source], d_send.at[0], d_recv.at[source], (kv, owner))

        @pl.when(source != x)
        def _():
            copy.wait_recv()

        own = hid[source]
        for side in range(2):
            part = jnp.dot(own, down[side], preferred_element_type=F32).astype(BF16)
            esend[k, side] = part.reshape(2, R, CH)
            for dz in range(2):
                dy = 2 * k + odd
                copy = send(esend.at[k, side, dz], ebuf.at[dy, dz], e_send.at[k, side, dz], e_recv.at[dy, dz],
                            row_peer(dz, 2 * Y - dy, side))
                away = jnp.logical_not((odd == 0) & (core == side)) if k == 0 and dz == 0 else None
                e_copies.append((away, copy))
                if away is None:
                    copy.start()
                else:
                    pl.when(away)(copy.start)

                    @pl.when(jnp.logical_not(away))
                    def _():
                        ebuf[0, 0] = part[:R]

    total = resid.astype(F32)
    for dy in near_first(Y):
        for dz in range(2):
            copy = send(esend.at[0, 0, dz], ebuf.at[dy, dz], e_send.at[0, 0, dz], e_recv.at[dy, dz], partner)
            if dz or dy:
                copy.wait_recv()
            else:
                pl.when(jnp.logical_not(at_home))(copy.wait_recv)
    for dy in range(Y):
        for dz in range(2):
            total += ebuf[dy, dz].astype(F32)
    outv[...] = total.astype(BF16)

    for copy in [*a_copies, *m_copies, *d_copies, gain_copy]:
        copy.wait_send()
    for dy in range(Y):
        for dz in range(2):
            if dz or dy:
                row_copy(dy, dz).wait_send()
    pl.when(jnp.logical_not(at_home))(row_copy(0, 0).wait_send)
    for owner, copy in c_copies:
        pl.when(owner != t)(copy.wait_send)
    for away, copy in e_copies:
        if away is None:
            copy.wait_send()
        else:
            pl.when(away)(copy.wait_send)
    for piece in range(2):
        for up in range(2):
            direct(piece, up).wait_send()
            pl.when(middle)(relay(piece, up).wait_send)
        for slot in range(S):
            forward(piece, slot).wait_send()


def store(*refs):
    sem = refs[-1]
    copies = [pltpu.make_async_copy(refs[i], refs[4 + i], sem.at[i]) for i in range(4)]
    for copy in copies:
        copy.start()
    for copy in copies:
        copy.wait()


def per_device(Z, Y, T, *args):
    (tokens, norm_gain, w_query, w_key, w_value, w_outgate, w_input_gate, w_forget_gate,
     memory, normalizer, memory_max, w_output, ffn_gain, w_gate, w_up, w_down) = args
    R, CH = tokens.shape
    width, HD = w_query.shape
    heads = w_input_gate.shape[1]
    inner = w_output.shape[0]
    SHARD = w_down.shape[0]
    S = Z // 2
    PAD = -(-(SHARD + 2) // 32) * 32
    GH = S * PAD
    any_spec = pl.BlockSpec(memory_space=pl.ANY)
    dma = pltpu.SemaphoreType.DMA
    outs = (
        jax.ShapeDtypeStruct((R, CH), BF16),
        jax.ShapeDtypeStruct((R, HD, HD), F32),
        jax.ShapeDtypeStruct((R, 1, HD), F32),
        jax.ShapeDtypeStruct((1, R), F32),
    )
    held = pl.pallas_call(
        functools.partial(kernel, Z, Y, T, S, SHARD, PAD),
        name="layer",
        out_shape=tuple(pltpu.VMEM(o.shape, o.dtype) for o in outs),
        in_specs=[any_spec] * 16,
        out_specs=(pl.BlockSpec(memory_space=pltpu.VMEM),) * 4,
        scratch_shapes=[
            pltpu.VMEM((T, R, CH), BF16),
            pltpu.VMEM((1, width), F32),
            pltpu.VMEM((width, 4 * HD), BF16),
            pltpu.VMEM((2, heads, width), BF16),
            pltpu.VMEM((R, HD, HD), F32),
            pltpu.VMEM((R, 1, HD), F32),
            pltpu.VMEM((1, R), F32),
            pltpu.VMEM((inner, CH), BF16),
            pltpu.VMEM((2, 1, CH), F32),
            pltpu.VMEM((2, 3, S, PAD, CH), BF16),
            pltpu.VMEM((R, HD), F32),
            pltpu.VMEM((T, R, HD), BF16),
            pltpu.VMEM((R, CH), BF16),
            pltpu.VMEM((Y // 2, 2, 2, R, CH), BF16),
            pltpu.VMEM((Y // 2, 2 * R, 2 * GH), BF16),
            pltpu.VMEM((T // 2, 2 * R, 2 * GH), BF16),
            pltpu.VMEM((T // 2, 2 * R, GH), BF16),
            pltpu.VMEM((Y // 2, 2, 2, R, CH), BF16),
            pltpu.VMEM((Y, 2, R, CH), BF16),
            dma((16,)), pltpu.SemaphoreType.REGULAR, pltpu.SemaphoreType.REGULAR((2,)),
            dma((T,)), dma((T,)), dma((2, 2)), dma((2, S)), dma((2, 2)), dma((2,)), dma((2, S)), dma((2, S)), dma, dma,
            dma((T,)), dma((T,)), dma((Y, 2)), dma((Y // 2, 2, 2)), dma((Y // 2,)), dma((T // 2,)),
            dma((T // 2,)), dma((T // 2,)), dma((Y // 2, 2, 2)), dma((Y, 2)),
        ],
        compiler_params=pltpu.CompilerParams(collective_id=0, has_side_effects=True),
    )(
        tokens, norm_gain.reshape(1, width), w_query, w_key, w_value, w_outgate,
        w_input_gate.T, w_forget_gate.T, memory.reshape(R, HD, HD), normalizer, memory_max.T,
        w_output, ffn_gain.reshape(1, CH), w_gate.T, w_up.T, w_down,
    )
    result, new_memory, new_normalizer, new_max = pl.pallas_call(
        store,
        name="store",
        out_shape=outs,
        in_specs=[pl.BlockSpec(memory_space=pltpu.VMEM)] * 4,
        out_specs=(any_spec,) * 4,
        scratch_shapes=[dma((4,))],
    )(*[pltpu.with_memory_space_constraint(h, pltpu.VMEM) for h in held])
    return result, new_memory.reshape(R, 1, HD, HD), new_normalizer, new_max.T


def solution(mesh):
    placed = (
        P("kv", "tp"), P(),
        P(None, "tp"), P(None, "tp"), P(None, "tp"), P(None, "tp"),
        P(), P(),
        P("kv", "tp", None, None), P("kv", "tp", None), P("kv", "tp"),
        P(None, "tp"), P("tp"), P("tp", "kv"), P("tp", "kv"), P("kv", "tp"),
    )
    T = mesh.shape["tp"]
    Z, Y = mesh.shape["kv"] // T, T
    return jax.shard_map(
        functools.partial(per_device, Z, Y, T),
        mesh=mesh,
        in_specs=placed,
        out_specs=(P("kv", "tp"), P("kv", "tp", None, None), P("kv", "tp", None), P("kv", "tp")),
        check_vma=False,
    )
```
